32 devices in a mesh: fs: 8 (over z, core), tp: 4 (over y, x).
Axes of the slice: x: 2, y: 2, z: 4, core: 2. Of those that a mesh axis runs over, the one named last changes fastest.
Arguments:
- tokens: bfloat16 [1024, 2048], P('fs'), may hold values from -6 to 6
- experts: int32 [1024, 4], P('fs'), may hold values from 0 to 7, all different within a row; in each aligned block of 128 rows (0 to 127, 128 to 255, ...) at most 96 rows name the same one
- routing: float32 [1024, 4], P('fs'), may hold values from 0.05 to 0.6
- norm_gain: float32 [2048], replicated, may hold values from 0.1 to 1.9
- gate_master: float32 [8, 2048, 2048], P(None, 'fs', 'tp'), may hold values from -0.625 to 0.625
- linear_master: float32 [8, 2048, 2048], P(None, 'fs', 'tp'), may hold values from -0.625 to 0.625
- down_weight: bfloat16 [8, 2048, 2048], P('fs', None, 'tp'), may hold values from -0.013671875 to 0.013671875
Outputs:
- gate_out: bfloat16 [8, 2048, 2048], P('fs', None, 'tp')
- linear_out: bfloat16 [8, 2048, 2048], P('fs', None, 'tp')
- expert_mix: bfloat16 [1024, 2048], P('fs', 'tp')
The draws below stay inside these ranges and needn't reach their ends.
Inputs may be any that keep to these rules, and one draw needn't show every extreme that they name: Each row names 4 different experts; within the rows of one index of fs (aligned blocks of 128 rows) no expert is named by more than 96 rows, and in some blocks some expert is named by exactly 96; every expert is named somewhere.
All inputs are finite; a program needn't handle non-finite values.
Results may differ from the reference program's by a relative error of at most 0.023.
Values may be sent and summed in bfloat16 or wider, within the bound.
No kernel may reach another device: no remote copies, remote signals or barrier semaphores. Data moves between devices by JAX's collectives and lax.ppermute only.
A program may use at most 64 MiB of HBM per device.

```python
import math
import jax
import jax.numpy as jnp
import numpy as np
from jax import lax

D = 2048
DE = 2048
TOP = 4
TOK_DEV = 128
EXPERTS = 8
HID_DEV = 512
CAP = 96
TOKENS = 1024
N_TP = 4


def levels(key, dims, shards, smallest, largest):
    level = 1.0
    for position, blocks in shards:
        draws = jax.random.uniform(jax.random.fold_in(jax.random.fold_in(key, 6), position), (blocks,), jnp.float32, smallest / len(shards), largest / len(shards))
        level = level * jnp.repeat(jnp.exp(draws), dims[position] // blocks).reshape((-1,) + (1,) * (len(dims) - 1 - position))
    return level


def assign_block(own_key, own, number, rows, count, top, most, lean):
    sequence = jax.random.permutation(own_key, count)
    packed, usual = shares(count, rows * top, most, lean, True), shares(count, rows * top, most, lean, False)
    places = jnp.arange(count)

    def named(tallies, offset_by):
        used = int((tallies > 0).sum())
        fixed = max(1, used // 4)
        moved = fixed + (places - fixed + offset_by * (used - fixed)) % max(1, count - fixed)
        return jnp.zeros((count,), jnp.int32).at[sequence[jnp.where(places < fixed, places, moved)]].set(jnp.asarray(tallies, jnp.int32))

    tallies = jnp.where(number % 4 == 0, named(packed, number // 4), named(usual, number - number // 4 - 1))
    mixed = jax.random.permutation(jax.random.fold_in(own, 3), count)
    donor, sink = mixed[0:count // 2 * 2:2], mixed[1:count // 2 * 2:2]
    room = jnp.minimum(tallies[donor] - 1, most - tallies[sink]) // 2
    room = jnp.where((donor == sequence[0]) | (sink == sequence[0]) | (tallies[sink] == 0), 0, jnp.maximum(room, 0))
    moved = jax.random.randint(jax.random.fold_in(own, 4), (count // 2,), 0, 1 << 20) % (room + 1)
    tallies = tallies.at[donor].add(-moved).at[sink].add(moved)
    labels = jnp.searchsorted(jnp.cumsum(tallies), jnp.arange(rows * top), side="right").astype(jnp.int32)
    listing = labels.reshape(top, rows).T
    listing = listing[jax.random.permutation(jax.random.fold_in(own, 1), rows)]
    offset_by = jax.random.randint(jax.random.fold_in(own, 2), (rows, 1), 0, top)
    return jnp.take_along_axis(listing, (jnp.arange(top)[None, :] + offset_by) % top, axis=1)


def shares(number_of, total, limit, lean, full):
    loads = [(1 << 20) // math.isqrt(rank ** lean) + 1 for rank in range(1, number_of + 1)]
    largest = limit if full else min(limit, max(-(-total // number_of), total * loads[0] // sum(loads)))
    least = 1 if total - largest >= number_of - 1 else 0
    given, surplus = [largest] + [least] * (number_of - 1), total - largest - least * (number_of - 1)
    while surplus > 0:
        movable = [i for i in range(1, number_of) if given[i] < largest] or [i for i in range(1, number_of) if given[i] < limit]
        mass, budget = sum([loads[i] for i in movable]), surplus
        for i in movable:
            extra = min(limit - given[i], max(1, budget * loads[i] // mass), surplus)
            given[i] = given[i] + extra
            surplus = surplus - extra
    return np.array(given)


def centred(stream_key, shape, scale, bound, shards=(), kind=jnp.bfloat16):
    loudness = levels(stream_key, shape, shards, -0.22, 0.18) if shards else 1.0
    entries = jax.random.normal(stream_key, shape, jnp.float32) * scale * loudness
    return jnp.minimum(jnp.maximum(entries, -bound), bound).astype(kind)


def setup_inputs(seed: int = 0) -> dict:
    key_list = jax.random.split(jax.random.key(seed), 8)
    tokens = centred(key_list[0], (TOKENS, D), 1.0, 6.0, ((0, 8),))
    experts_keys = jax.random.split(jax.random.fold_in(key_list[1], 1), TOKENS // TOK_DEV)
    experts_turns = jax.random.permutation(jax.random.fold_in(key_list[1], 3), TOKENS // TOK_DEV)
    experts = jax.vmap(lambda own, number: assign_block(jax.random.fold_in(key_list[1], 2), own, number, TOK_DEV, EXPERTS, TOP, CAP, 0))(experts_keys, experts_turns).reshape((TOKENS, TOP))
    routing = jnp.clip(0.05 + 0.55 * jax.random.uniform(key_list[2], (TOKENS, TOP), jnp.float32) ** levels(key_list[2], (TOKENS, TOP), ((0, 8),), -0.2, 0.2), 0.05, 0.6)
    norm_gain = jnp.clip(1.0 + 0.18 * jax.random.normal(key_list[3], (D,), jnp.float32), 0.1, 1.9)
    gate_master = centred(key_list[4], (EXPERTS, D, DE), (D // 25) ** -0.5, 0.625, ((1, 8), (2, 4)), jnp.float32)
    linear_master = centred(key_list[5], (EXPERTS, D, DE), (D // 25) ** -0.5, 0.625, ((1, 8), (2, 4)), jnp.float32)
    down_weight = centred(key_list[6], (EXPERTS, D, DE), (DE * 100) ** -0.5, 0.013671875, ((0, 8), (2, 4)))
    return dict(tokens=tokens, experts=experts, routing=routing, norm_gain=norm_gain, gate_master=gate_master, linear_master=linear_master, down_weight=down_weight)


clamp_limit = 7.0
gate_slope = 1.702


def reference(tokens, experts, routing, norm_gain, gate_master, linear_master, down_weight):
    gain_col = norm_gain[None, :, None]
    gate_out = (gate_master * gain_col).astype(jnp.bfloat16)
    linear_out = (linear_master * gain_col).astype(jnp.bfloat16)
    flat_ids = experts.reshape(-1)
    owner = jnp.arange(TOKENS * TOP, dtype=jnp.int32) // TOP
    weights = routing.reshape(-1)
    span_rows = CAP * EXPERTS

    def one_expert(running, expert_id):
        pick_order = jnp.argsort((flat_ids != expert_id).astype(jnp.int32), stable=True)[:span_rows]
        in_use = flat_ids[pick_order] == expert_id
        row_owner = owner[pick_order]
        row_data = tokens[row_owner]
        pre_gate = jnp.dot(row_data, gate_out[expert_id], preferred_element_type=jnp.float32)
        pre_linear = jnp.dot(row_data, linear_out[expert_id], preferred_element_type=jnp.float32)
        clamped = jnp.minimum(pre_gate, clamp_limit)
        active = (clamped * jax.nn.sigmoid(gate_slope * clamped)
                  * (jnp.clip(pre_linear, -clamp_limit, clamp_limit) + 1.0)).astype(jnp.bfloat16)
        blocks = active.astype(jnp.float32).reshape(span_rows, N_TP, HID_DEV)
        down_blocks = down_weight[expert_id].astype(jnp.float32).reshape(D, N_TP, HID_DEV)
        block_part = jnp.einsum("rbh,dbh->rbd", blocks, down_blocks)
        rounded = lax.optimization_barrier(block_part.astype(jnp.bfloat16)).astype(jnp.float32)
        total = jnp.sum(rounded, axis=1)
        scale_rows = jnp.where(in_use, weights[pick_order], jnp.float32(0.0))
        running = running.at[row_owner].add(total * scale_rows[:, None])
        return running, None

    start = jnp.zeros((TOKENS, D), jnp.float32)
    final, _ = lax.scan(one_expert, start, jnp.arange(EXPERTS, dtype=jnp.int32))
    return (gate_out, linear_out, final.astype(jnp.bfloat16))
```

```python
import jax
import jax.numpy as jnp
from jax import lax
from jax.experimental import pallas as pl
from jax.experimental.pallas import tpu as pltpu
from jax.sharding import PartitionSpec as P

clamp_limit = 7.0
gate_slope = 1.702
lanes = 128


HBM = pl.BlockSpec(memory_space=pl.ANY)
VMEM = pl.BlockSpec(memory_space=pltpu.VMEM)
SMEM = pl.BlockSpec(memory_space=pltpu.SMEM)


def swap(value, axis, size, step):
    return lax.ppermute(value, axis, [(i, i ^ step) for i in range(size)])


def chunk_widths(hidden):
    count = hidden // lanes
    if count >= 3:
        return [hidden - 2 * lanes, lanes, lanes]
    return [lanes] * count


def grant(used):
    return pltpu.CompilerParams(vmem_limit_bytes=min(used + (8 << 20), 60 << 20))


def cost(flops, moved):
    return pl.CostEstimate(flops=flops, bytes_accessed=moved, transcendentals=0)


def convert(place, gain_col, gate_master, linear_master, widths):
    experts, rows, hidden = gate_master.shape
    kinds = len(widths)

    def kernel(place_ref, gain_ref, gate_ref, linear_ref, *refs):
        outs = refs[: kinds * experts]
        gate_buf, linear_buf = refs[kinds * experts : kinds * experts + 2]
        bufs = refs[kinds * experts + 2 : kinds * experts + 2 + kinds]
        in_sem, out_sem = refs[-2:]
        me = place_ref[0]
        loads = []
        for k in range(experts):
            pair = [
                pltpu.make_async_copy(gate_ref.at[me ^ k], gate_buf.at[k], in_sem.at[0, k]),
                pltpu.make_async_copy(linear_ref.at[me ^ k], linear_buf.at[k], in_sem.at[1, k]),
            ]
            order = pair
            for copy in order:
                copy.start()
            loads.append(pair)
        gain = gain_ref[...]
        stores = []
        for k in range(experts):
            for copy in loads[k]:
                copy.wait()
            offset = 0
            for c, width in enumerate(widths):
                span = slice(offset, offset + width)
                bufs[c][k, :, :width] = (gate_buf[k, :, span] * gain).astype(jnp.bfloat16)
                bufs[c][k, :, width:] = (linear_buf[k, :, span] * gain).astype(jnp.bfloat16)
                offset += width
                copy = pltpu.make_async_copy(bufs[c].at[k], outs[c * experts + k], out_sem.at[c, k])
                copy.start()
                stores.append(copy)
        for copy in stores:
            copy.wait()

    outs = pl.pallas_call(
        kernel,
        out_shape=[
            jax.ShapeDtypeStruct((rows, 2 * width), jnp.bfloat16) for width in widths for _ in range(experts)
        ],
        in_specs=[SMEM, VMEM, HBM, HBM],
        out_specs=[HBM] * (kinds * experts),
        scratch_shapes=[
            pltpu.VMEM((experts, rows, hidden), jnp.float32),
            pltpu.VMEM((experts, rows, hidden), jnp.float32),
            *[pltpu.VMEM((experts, rows, 2 * width), jnp.bfloat16) for width in widths],
            pltpu.SemaphoreType.DMA((2, experts)),
            pltpu.SemaphoreType.DMA((kinds, experts)),
        ],
        cost_estimate=cost(4 * experts * rows * hidden, 12 * experts * rows * hidden),
        name="convert",
    )(place, gain_col, gate_master, linear_master)
    return [outs[c * experts : (c + 1) * experts] for c in range(kinds)]


def activate(place, halves, pieces, built, offset, hidden):
    count = len(pieces)
    rows, width = pieces[0].shape[0], pieces[0].shape[1] // 2
    half, depth = halves[0].shape
    total = 2 * half
    block = min(512, half)

    def kernel(place_ref, xa_ref, xb_ref, *refs):
        piece_refs = refs[:count]
        active_ref, gate_ref, linear_ref, w_buf, o_sem = refs[count + len(built) :]
        me = place_ref[0]
        for k in range(count):
            row = pl.multiple_of((me ^ k) * rows, rows)
            w_buf[pl.ds(row, rows), :] = piece_refs[k][...]
        out_copies = [
            pltpu.make_async_copy(
                w_buf.at[:, pl.ds(s * width, width)], ref.at[:, pl.ds(offset, width)], o_sem.at[s]
            )
            for s, ref in enumerate((gate_ref, linear_ref))
        ]
        for copy in out_copies:
            copy.start()
        for h, x_ref in enumerate((xa_ref, xb_ref)):
            for n in range(half // block):
                pre = jnp.dot(
                    x_ref[pl.ds(n * block, block), :], w_buf[...], preferred_element_type=jnp.float32
                )
                clamped = jnp.minimum(pre[:, :width], clamp_limit)
                linear = jnp.clip(pre[:, width:], -clamp_limit, clamp_limit) + 1.0
                active_ref[pl.ds(h * half + n * block, block), :] = (
                    clamped * jax.nn.sigmoid(gate_slope * clamped) * linear
                ).astype(jnp.bfloat16)
        for copy in out_copies:
            copy.wait()

    out = jax.ShapeDtypeStruct((count * rows, hidden), jnp.bfloat16)
    return pl.pallas_call(
        kernel,
        out_shape=[jax.ShapeDtypeStruct((total, width), jnp.bfloat16), out, out],
        in_specs=[SMEM, VMEM, VMEM] + [VMEM] * count + [HBM] * len(built),
        out_specs=[VMEM, HBM, HBM],
        input_output_aliases={3 + count + n: 1 + n for n in range(len(built))},
        scratch_shapes=[
            pltpu.VMEM((count * rows, 2 * width), jnp.bfloat16),
            pltpu.SemaphoreType.DMA((2,)),
        ],
        compiler_params=grant(total * depth * 2 + 4 * count * rows * width * 2 + 2 * total * width * 6),
        cost_estimate=cost(4 * total * depth * width, 2 * total * depth),
        name="activate",
    )(place, *halves, *pieces, *built)


def assemble(place, shares):
    groups, sub, width = shares[0].shape
    parts = len(shares)

    def kernel(place_ref, *refs):
        for q in range(parts):
            row = pl.multiple_of((place_ref[1] ^ q) * sub, sub)
            for g in range(groups):
                refs[-1][g, pl.ds(row, sub), :] = refs[q][g]

    return pl.pallas_call(
        kernel,
        out_shape=jax.ShapeDtypeStruct((groups, parts * sub, width), shares[0].dtype),
        in_specs=[SMEM] + [VMEM] * parts,
        out_specs=VMEM,
        compiler_params=grant(4 * groups * parts * sub * width),
        cost_estimate=cost(groups * parts * sub * width, 4 * groups * parts * sub * width),
        name="assemble",
    )(place, *shares)


def project(actives, downs, offsets, running, scale):
    count, chunks = len(downs), len(actives)
    total = actives[0][0].shape[0]
    features = downs[0].shape[0]
    widths = [group[0].shape[1] for group in actives]
    block = min(256, total)
    blocks = total // block
    extra = ([running] if running is not None else []) + ([scale] if scale is not None else [])

    def kernel(*refs):
        active_refs = [refs[c * count : (c + 1) * count] for c in range(chunks)]
        down_refs = refs[chunks * count : (chunks + 1) * count]
        others = refs[(chunks + 1) * count :]
        sides = [
            jnp.concatenate([d[:, o : o + w] for d in down_refs], axis=1) for o, w in zip(offsets, widths)
        ]
        for n in range(blocks):
            span = slice(n * block, (n + 1) * block)
            acc = others[0][span, :] if running is not None else None
            for c in range(chunks):
                left = jnp.concatenate([a[span, :] for a in active_refs[c]], axis=1)
                part = lax.dot_general(
                    left, sides[c], (((1,), (1,)), ((), ())), preferred_element_type=jnp.float32
                )
                acc = part if acc is None else acc + part
            if scale is None:
                others[-1][span, :] = acc
            else:
                acc = acc * others[len(extra) - 1][span, :]
                if n < blocks // 2:
                    others[-2][span, :] = acc
                else:
                    others[-1][slice(n * block - total // 2, (n + 1) * block - total // 2), :] = acc.astype(
                        jnp.bfloat16
                    )

    if scale is None:
        shapes = jax.ShapeDtypeStruct((total, features), jnp.float32)
        specs = VMEM
    else:
        shapes = [
            jax.ShapeDtypeStruct((total // 2, features), jnp.float32),
            jax.ShapeDtypeStruct((total // 2, features), jnp.bfloat16),
        ]
        specs = [VMEM, VMEM]
    return pl.pallas_call(
        kernel,
        out_shape=shapes,
        in_specs=[VMEM] * ((chunks + 1) * count + len(extra)),
        out_specs=specs,
        compiler_params=grant(
            2 * count * total * sum(widths) + 4 * features * sum(d.shape[1] for d in downs) + 12 * total * features
        ),
        cost_estimate=cost(2 * total * features * count * sum(widths), 4 * total * features),
        name="project",
    )(*[a for group in actives for a in group], *downs, *extra)


def combine(kept, arrived, groups):
    total, features = kept.shape
    each = total // groups

    def kernel(kept_ref, arrived_ref, *outs):
        for g in range(groups):
            span = slice(g * each, (g + 1) * each)
            value = kept_ref[span, :] + arrived_ref[span, :].astype(jnp.float32)
            outs[g][...] = value.astype(outs[g].dtype)

    return pl.pallas_call(
        kernel,
        out_shape=[
            jax.ShapeDtypeStruct((each, features), jnp.bfloat16 if g else jnp.float32) for g in range(groups)
        ],
        in_specs=[VMEM, VMEM],
        out_specs=[VMEM] * groups,
        compiler_params=grant(12 * total * features),
        cost_estimate=cost(total * features, 8 * total * features),
        name="combine",
    )(kept, arrived)


def solution(mesh):
    n_fs, n_tp = mesh.shape["fs"], mesh.shape["tp"]
    n_z = n_fs // 2

    def on_device(tokens, experts, routing, norm_gain, gate_master, linear_master, down_weight):
        tok_count, width = tokens.shape
        expert_count, rows, hidden = gate_master.shape
        sub = tok_count // n_tp
        features = width // n_tp
        i, j = lax.axis_index("fs"), lax.axis_index("tp")
        place = jnp.stack([i, j]).astype(jnp.int32)

        share = lax.dynamic_slice_in_dim(tokens, j * sub, sub, 0)
        shares = jnp.stack([share] + [swap(share, "fs", n_fs, 2 * k) for k in range(1, n_z)])
        near = assemble(place, [shares] + [swap(shares, "tp", n_tp, q) for q in range(1, n_tp)])
        near = near.reshape(n_z * tok_count, width)
        far = swap(near, "fs", n_fs, 1)

        down_blocks = down_weight.reshape(n_tp, features, hidden)
        picked = [lax.dynamic_index_in_dim(down_blocks, j ^ q, 0, keepdims=False) for q in range(n_tp)]
        downs = [picked[0]] + [swap(picked[q], "tp", n_tp, q) for q in range(1, n_tp)]

        chosen = experts[:, :, None] == jnp.arange(expert_count, dtype=jnp.int32)[None, None, :]
        mixing = jnp.sum(jnp.where(chosen, routing[:, :, None], 0.0), axis=1).T
        mixing = jnp.stack([mixing] + [swap(mixing, "fs", n_fs, 2 * k) for k in range(1, n_z)])
        mixing = jnp.stack([mixing, swap(mixing, "fs", n_fs, 1)])
        scale = lax.dynamic_index_in_dim(mixing, i, 2, keepdims=False).reshape(-1, 1)

        widths = chunk_widths(hidden)
        offsets = [sum(widths[:c]) for c in range(len(widths))]
        gain_col = lax.dynamic_slice_in_dim(norm_gain, i * rows, rows, 0).reshape(rows, 1)
        pieces = convert(place, gain_col, gate_master, linear_master, widths)
        arrived = [[group[0]] + [swap(group[k], "fs", n_fs, k) for k in range(1, n_fs)] for group in pieces]

        built = []
        actives = []
        running = None
        for c in range(len(widths)):
            active, *built = activate(place, [near, far], arrived[c], built, offsets[c], hidden)
            actives.append([active] + [swap(active, "tp", n_tp, q) for q in range(1, n_tp)])

        if len(widths) > 1:
            running = project(actives[:-1], downs, offsets[:-1], None, None)
        kept, sent = project(actives[-1:], downs, offsets[-1:], running, scale)
        own, *others = combine(kept, swap(sent, "fs", n_fs, 1), n_z)
        total = own
        for k, other in enumerate(others, 1):
            total = total + swap(other, "fs", n_fs, 2 * k).astype(jnp.float32)
        return built[0][None], built[1][None], total.astype(jnp.bfloat16)

    placed = (
        P("fs", None),
        P("fs", None),
        P("fs", None),
        P(),
        P(None, "fs", "tp"),
        P(None, "fs", "tp"),
        P("fs", None, "tp"),
    )
    return jax.shard_map(
        on_device,
        mesh=mesh,
        in_specs=placed,
        out_specs=(P("fs", None, "tp"), P("fs", None, "tp"), P("fs", "tp")),
        check_vma=False,
    )
```

```python
import jax
import jax.numpy as jnp
from jax import lax
from jax.experimental import pallas as pl
from jax.experimental.pallas import tpu as pltpu
from jax.sharding import PartitionSpec as P

clamp_limit = 7.0
gate_slope = 1.702
lanes = 128


HBM = pl.BlockSpec(memory_space=pltpu.HBM)
VMEM = pl.BlockSpec(memory_space=pltpu.VMEM)
SMEM = pl.BlockSpec(memory_space=pltpu.SMEM)


def swap(value, axis, size, step):
    return lax.ppermute(value, axis, [(i, i ^ step) for i in range(size)])


def chunk_widths(hidden):
    return [lanes] * (hidden // lanes)


def grant(used):
    return pltpu.CompilerParams(vmem_limit_bytes=min(used + (8 << 20), 60 << 20))


def cost(flops, moved):
    return pl.CostEstimate(flops=flops, bytes_accessed=moved, transcendentals=0)


def convert(place, gain_col, gate_master, linear_master, widths):
    experts, rows, hidden = gate_master.shape
    kinds = len(widths)

    def kernel(place_ref, gain_ref, gate_ref, linear_ref, *refs):
        outs = refs[: kinds * experts]
        gate_buf, linear_buf = refs[kinds * experts : kinds * experts + 2]
        bufs = refs[kinds * experts + 2 : kinds * experts + 2 + kinds]
        in_sem, out_sem = refs[-2:]
        me = place_ref[0]
        loads = []
        for k in range(experts):
            pair = [
                pltpu.make_async_copy(gate_ref.at[me ^ k], gate_buf.at[k], in_sem.at[0, k]),
                pltpu.make_async_copy(linear_ref.at[me ^ k], linear_buf.at[k], in_sem.at[1, k]),
            ]
            order = pair
            for copy in order:
                copy.start()
            loads.append(pair)
        gain = gain_ref[...]
        stores = []
        for k in range(experts):
            for copy in loads[k]:
                copy.wait()
            offset = 0
            for c, width in enumerate(widths):
                span = slice(offset, offset + width)
                bufs[c][k, :, :width] = (gate_buf[k, :, span] * gain).astype(jnp.bfloat16)
                bufs[c][k, :, width:] = (linear_buf[k, :, span] * gain).astype(jnp.bfloat16)
                offset += width
                copy = pltpu.make_async_copy(bufs[c].at[k], outs[c * experts + k], out_sem.at[c, k])
                copy.start()
                stores.append(copy)
        for copy in stores:
            copy.wait()

    outs = pl.pallas_call(
        kernel,
        out_shape=[
            jax.ShapeDtypeStruct((rows, 2 * width), jnp.bfloat16) for width in widths for _ in range(experts)
        ],
        in_specs=[SMEM, VMEM, HBM, HBM],
        out_specs=[HBM] * (kinds * experts),
        scratch_shapes=[
            pltpu.VMEM((experts, rows, hidden), jnp.float32),
            pltpu.VMEM((experts, rows, hidden), jnp.float32),
            *[pltpu.VMEM((experts, rows, 2 * width), jnp.bfloat16) for width in widths],
            pltpu.SemaphoreType.DMA((2, experts)),
            pltpu.SemaphoreType.DMA((kinds, experts)),
        ],
        cost_estimate=cost(4 * experts * rows * hidden, 12 * experts * rows * hidden),
        name="convert",
    )(place, gain_col, gate_master, linear_master)
    return [outs[c * experts : (c + 1) * experts] for c in range(kinds)]


def activate(place, halves, pieces, built, offset, hidden):
    count = len(pieces)
    rows, width = pieces[0].shape[0], pieces[0].shape[1] // 2
    half, depth = halves[0].shape
    total = 2 * half
    block = min(512, half)

    def kernel(place_ref, xa_ref, xb_ref, *refs):
        piece_refs = refs[:count]
        active_ref, gate_ref, linear_ref, w_buf, o_sem = refs[count + len(built) :]
        me = place_ref[0]
        for k in range(count):
            row = pl.multiple_of((me ^ k) * rows, rows)
            w_buf[pl.ds(row, rows), :] = piece_refs[k][...]
        out_copies = [
            pltpu.make_async_copy(
                w_buf.at[:, pl.ds(s * width, width)], ref.at[:, pl.ds(offset, width)], o_sem.at[s]
            )
            for s, ref in enumerate((gate_ref, linear_ref))
        ]
        for copy in out_copies:
            copy.start()
        for h, x_ref in enumerate((xa_ref, xb_ref)):
            for n in range(half // block):
                pre = jnp.dot(
                    x_ref[pl.ds(n * block, block), :], w_buf[...], preferred_element_type=jnp.float32
                )
                clamped = jnp.minimum(pre[:, :width], clamp_limit)
                linear = jnp.clip(pre[:, width:], -clamp_limit, clamp_limit) + 1.0
                active_ref[pl.ds(h * half + n * block, block), :] = (
                    clamped * jax.nn.sigmoid(gate_slope * clamped) * linear
                ).astype(jnp.bfloat16)
        for copy in out_copies:
            copy.wait()

    out = jax.ShapeDtypeStruct((count * rows, hidden), jnp.bfloat16)
    return pl.pallas_call(
        kernel,
        out_shape=[jax.ShapeDtypeStruct((total, width), jnp.bfloat16), out, out],
        in_specs=[SMEM, VMEM, VMEM] + [VMEM] * count + [HBM] * len(built),
        out_specs=[VMEM, HBM, HBM],
        input_output_aliases={3 + count + n: 1 + n for n in range(len(built))},
        scratch_shapes=[
            pltpu.VMEM((count * rows, 2 * width), jnp.bfloat16),
            pltpu.SemaphoreType.DMA((2,)),
        ],
        compiler_params=grant(total * depth * 2 + 4 * count * rows * width * 2 + 2 * total * width * 6),
        cost_estimate=cost(4 * total * depth * width, 2 * total * depth),
        name="activate",
    )(place, *halves, *pieces, *built)


def assemble(place, shares):
    groups, sub, width = shares[0].shape
    parts = len(shares)

    def kernel(place_ref, *refs):
        for q in range(parts):
            row = pl.multiple_of((place_ref[1] ^ q) * sub, sub)
            for g in range(groups):
                refs[-1][g, pl.ds(row, sub), :] = refs[q][g]

    return pl.pallas_call(
        kernel,
        out_shape=jax.ShapeDtypeStruct((groups, parts * sub, width), shares[0].dtype),
        in_specs=[SMEM] + [VMEM] * parts,
        out_specs=VMEM,
        compiler_params=grant(4 * groups * parts * sub * width),
        cost_estimate=cost(groups * parts * sub * width, 4 * groups * parts * sub * width),
        name="assemble",
    )(place, *shares)


def load_sides(down_refs, sides, sems, offsets):
    loads = []
    for c, offset in enumerate(offsets):
        width = sides[c].shape[1] // len(down_refs)
        for q, ref in enumerate(down_refs):
            copy = pltpu.make_async_copy(
                ref.at[:, pl.ds(offset, width)], sides[c].at[:, pl.ds(q * width, width)], sems.at[c, q]
            )
            copy.start()
            loads.append(copy)
    return loads


def contract(active_refs, span, side):
    left = jnp.concatenate([a[span, :] for a in active_refs], axis=1)
    return lax.dot_general(left, side, (((1,), (1,)), ((), ())), preferred_element_type=jnp.float32)


def project_early(actives, downs, scale, offsets, widths):
    count, chunks, early = len(downs), len(widths), len(actives)
    features = downs[0].shape[0]
    total = scale.shape[0]
    block = min(256, total)

    def kernel(*refs):
        groups = [refs[c * count : (c + 1) * count] for c in range(early)]
        down_refs = refs[early * count : (early + 1) * count]
        scale_ref = refs[(early + 1) * count]
        outs = refs[(early + 1) * count + 1 :][: len(shapes)]
        *sides, sems = refs[(early + 1) * count + 1 + len(shapes) :]
        loads = load_sides(down_refs, [*sides, *outs[: chunks - early]], sems, offsets)
        outs[chunks - early][...] = scale_ref[...]
        for copy in loads:
            copy.wait()
        if not early:
            return
        for n in range(total // block):
            span = slice(n * block, (n + 1) * block)
            acc = None
            for c in range(early):
                part = contract(groups[c], span, sides[c][...])
                acc = part if acc is None else acc + part
            outs[-1][span, :] = acc

    shapes = [jax.ShapeDtypeStruct((features, count * w), jnp.bfloat16) for w in widths[early:]]
    shapes.append(jax.ShapeDtypeStruct(scale.shape, jnp.float32))
    if early:
        shapes.append(jax.ShapeDtypeStruct((total, features), jnp.float32))
    return pl.pallas_call(
        kernel,
        out_shape=shapes,
        in_specs=[VMEM] * (early * count) + [HBM] * count + [VMEM],
        out_specs=[VMEM] * len(shapes),
        scratch_shapes=[
            *[pltpu.VMEM((features, count * w), jnp.bfloat16) for w in widths[:early]],
            pltpu.SemaphoreType.DMA((chunks, count)),
        ],
        compiler_params=grant(
            2 * count * total * sum(widths) + 2 * features * count * sum(widths) + 8 * total * features
        ),
        cost_estimate=cost(2 * total * features * count * sum(widths), 4 * total * features),
        name="project",
    )(*[a for group in actives for a in group], *downs, scale)


def project_late(actives, sides, running, scale):
    count, late = len(actives[0]), len(actives)
    total = actives[0][0].shape[0]
    features = sides[0].shape[0]
    block = min(256, total // 2)
    blocks = total // block
    depth = sum(side.shape[1] for side in sides)

    def kernel(*refs):
        groups = [refs[c * count : (c + 1) * count] for c in range(late)]
        side_refs = refs[late * count : late * count + late]
        scale_ref, *rest = refs[late * count + late :]
        kept_ref, sent_ref = rest[-2:]
        for n in reversed(range(blocks)):
            span = slice(n * block, (n + 1) * block)
            acc = rest[0][span, :] if running else None
            for c in range(late):
                part = contract(groups[c], span, side_refs[c][...])
                acc = part if acc is None else acc + part
            acc = acc * scale_ref[span, :]
            if n < blocks // 2:
                kept_ref[span, :] = acc
            else:
                sent_ref[slice(n * block - total // 2, (n + 1) * block - total // 2), :] = acc.astype(jnp.bfloat16)

    return pl.pallas_call(
        kernel,
        out_shape=[
            jax.ShapeDtypeStruct((total // 2, features), jnp.float32),
            jax.ShapeDtypeStruct((total // 2, features), jnp.bfloat16),
        ],
        in_specs=[VMEM] * (late * (count + 1) + 1 + len(running)),
        out_specs=[VMEM] * 2,
        compiler_params=grant(2 * total * depth + 2 * features * depth + 10 * total * features),
        cost_estimate=cost(2 * total * features * depth, 4 * total * features),
        name="project",
    )(*[a for group in actives for a in group], *sides, scale, *running)


def combine(kept, arrived, groups):
    total, features = kept.shape
    each = total // groups

    def kernel(kept_ref, arrived_ref, *outs):
        for g in range(groups):
            span = slice(g * each, (g + 1) * each)
            value = kept_ref[span, :] + arrived_ref[span, :].astype(jnp.float32)
            outs[g][...] = value.astype(outs[g].dtype)

    return pl.pallas_call(
        kernel,
        out_shape=[
            jax.ShapeDtypeStruct((each, features), jnp.bfloat16 if g else jnp.float32) for g in range(groups)
        ],
        in_specs=[VMEM, VMEM],
        out_specs=[VMEM] * groups,
        compiler_params=grant(12 * total * features),
        cost_estimate=cost(total * features, 8 * total * features),
        name="combine",
    )(kept, arrived)


def solution(mesh):
    n_fs, n_tp = mesh.shape["fs"], mesh.shape["tp"]
    n_z = n_fs // 2

    def on_device(tokens, experts, routing, norm_gain, gate_master, linear_master, down_weight):
        tok_count, width = tokens.shape
        expert_count, rows, hidden = gate_master.shape
        sub = tok_count // n_tp
        features = width // n_tp
        i, j = lax.axis_index("fs"), lax.axis_index("tp")
        place = jnp.stack([i, j]).astype(jnp.int32)

        share = lax.dynamic_slice_in_dim(tokens, j * sub, sub, 0)
        shares = jnp.stack([share] + [swap(share, "fs", n_fs, 2 * k) for k in range(1, n_z)])
        shares = [shares] + [swap(shares, "tp", n_tp, q) for q in range(1, n_tp)]
        near = assemble(place, shares)
        near = near.reshape(n_z * tok_count, width)
        far = swap(near, "fs", n_fs, 1)

        down_blocks = down_weight.reshape(n_tp, features, hidden)
        picked = [lax.dynamic_index_in_dim(down_blocks, j ^ q, 0, keepdims=False) for q in range(n_tp)]
        downs = [picked[0]] + [swap(picked[q], "tp", n_tp, q) for q in range(1, n_tp)]

        chosen = experts[:, :, None] == jnp.arange(expert_count, dtype=jnp.int32)[None, None, :]
        mixing = jnp.sum(jnp.where(chosen, routing[:, :, None], 0.0), axis=1).T
        mixing = jnp.stack([mixing] + [swap(mixing, "fs", n_fs, 2 * k) for k in range(1, n_z)])
        mixing = jnp.stack([mixing, swap(mixing, "fs", n_fs, 1)])
        scale = lax.dynamic_index_in_dim(mixing, i, 2, keepdims=False).reshape(-1, 1)

        widths = chunk_widths(hidden)
        offsets = [sum(widths[:c]) for c in range(len(widths))]
        gain_col = lax.dynamic_slice_in_dim(norm_gain, i * rows, rows, 0).reshape(rows, 1)
        pieces = convert(place, gain_col, gate_master, linear_master, widths)
        arrived = [[group[0]] + [swap(group[k], "fs", n_fs, k) for k in range(1, n_fs)] for group in pieces]

        built = []
        actives = []
        for c in range(len(widths)):
            active, *built = activate(place, [near, far], arrived[c], built, offsets[c], hidden)
            actives.append([active] + [swap(active, "tp", n_tp, q) for q in range(1, n_tp)])

        early = max(0, len(widths) - 2)
        rest = project_early(actives[:early], downs, scale, offsets, widths)
        sides, scale, running = rest[: len(widths) - early], rest[len(widths) - early], rest[len(widths) - early + 1 :]
        kept, sent = project_late(actives[early:], sides, running, scale)
        own, *others = combine(kept, swap(sent, "fs", n_fs, 1), n_z)
        total = own
        for k, other in enumerate(others, 1):
            total = total + swap(other, "fs", n_fs, 2 * k).astype(jnp.float32)
        return built[0][None], built[1][None], total.astype(jnp.bfloat16)

    placed = (
        P("fs", None),
        P("fs", None),
        P("fs", None),
        P(),
        P(None, "fs", "tp"),
        P(None, "fs", "tp"),
        P("fs", None, "tp"),
    )
    return jax.shard_map(
        on_device,
        mesh=mesh,
        in_specs=placed,
        out_specs=(P("fs", None, "tp"), P("fs", None, "tp"), P("fs", "tp")),
        check_vma=False,
    )
```
